32 devices in a mesh: sp: 8 (over z, y), tp: 4 (over x, core).
Axes of the slice: x: 2, y: 2, z: 4, core: 2. Of those that a mesh axis runs over, the one named last changes fastest.
Arguments:
- tokens: bfloat16 [6144, 2048], P(('sp', 'tp')), may hold values from -6 to 6
- norm_gain: float32 [2048], replicated, may hold values from 0.1 to 1.9
- w_query: bfloat16 [2048, 1024], P('sp', 'tp'), may hold values from -0.125 to 0.125
- w_forget: bfloat16 [2048, 1024], P('sp', 'tp'), may hold values from -0.125 to 0.125
- w_input: bfloat16 [2048, 1024], P('sp', 'tp'), may hold values from -0.125 to 0.125
- w_outgate: bfloat16 [2048, 1024], P('sp', 'tp'), may hold values from -0.125 to 0.125
- w_conv_value: bfloat16 [2048, 1024], P('sp', 'tp'), may hold values from -0.125 to 0.125
- w_conv_gate: bfloat16 [2048, 1024], P('sp', 'tp'), may hold values from -0.125 to 0.125
- w_gate_rec: bfloat16 [2048, 2048], P('sp', 'tp'), may hold values from -0.125 to 0.125
- w_gate_conv: bfloat16 [2048, 2048], P('sp', 'tp'), may hold values from -0.125 to 0.125
- lower_bound: float32 [1024], P('tp'), may hold values from 0.92 to 0.99991862, as said below
- decay_shift: float32 [6144, 1024], P('sp', 'tp'), may hold values from -0.7 to 0, as said below
- state_init: float32 [8, 128, 128], P('tp'), may hold values from -0.1875 to 0.1875
- head_gain: float32 [1024], P('tp'), may hold values from 0.1 to 1.9
- conv_kernel: float32 [31, 1024], P(None, 'tp'), may hold values from -7.5 to 7.5
- channel_gain: float32 [1024], P('tp'), may hold values from 0.1 to 1.9
- channel_bias: float32 [1024], P('tp'), may hold values from -3 to 3
- w_out_rec: bfloat16 [1024, 2048], P('tp', 'sp'), may hold values from -0.1875 to 0.1875
- w_out_conv: bfloat16 [1024, 2048], P('tp', 'sp'), may hold values from -0.1875 to 0.1875
Outputs:
- mixed_out: bfloat16 [6144, 2048], P('sp', 'tp')
The draws below stay inside these ranges and needn't reach their ends.
Inputs may be any that keep to these rules, and one draw needn't show every extreme that they name: `lower_bound`: every entry is below one. `decay_shift`: no entry is positive.
All inputs are finite; a program needn't handle non-finite values.
Results may differ from the reference program's by a relative error of at most 0.017.
Values may be sent and summed in bfloat16 or wider, within the bound.
No kernel may reach another device: no remote copies, remote signals or barrier semaphores. Data moves between devices by JAX's collectives and lax.ppermute only.
A program may use at most 64 MiB of HBM per device.

```python
import math
import jax
import jax.numpy as jnp
from jax import lax

D = 2048
HEADS = 8
HEAD = 128
CONV = 1024
KW = 31
BLOCK = 64
T_DEV = 768
HD = 1024
TOKENS = 6144


def draw_lower_bound(key, part):
    base_key = jax.random.fold_in(key, 11)
    head_key, slow_key, quick_seed = jax.random.split(base_key, 3)
    share = 0.5
    slow_heads = jax.random.uniform(head_key, (HEADS,), jnp.float32) < share
    slow_rate = jnp.exp(jax.random.uniform(slow_key, (HEADS, HEAD), jnp.float32, math.log(0.5), math.log(1.5))) / TOKENS
    fast_rate = jnp.exp(jax.random.uniform(quick_seed, (HEADS, HEAD), jnp.float32, math.log(0.03), math.log(0.08)))
    rate = jnp.where(slow_heads[:, None], slow_rate, fast_rate)
    return (1.0 - rate).reshape(HEADS * HEAD).astype(jnp.float32)


def draw_decay_shift(key, part):
    base_key = jax.random.fold_in(key, 23)
    block_key, position_key, depth_key = jax.random.split(base_key, 3)
    block_rate = jnp.exp(jax.random.uniform(block_key, (TOKENS // T_DEV,), jnp.float32, math.log(0.2), math.log(1.6)))
    starting_index = -jnp.repeat(block_rate, T_DEV) / TOKENS
    spots = jax.random.randint(position_key, (HEADS, 2), 0, TOKENS)
    places = jnp.arange(TOKENS, dtype=jnp.int32)
    dropped_sequence_items = jnp.any(places[:, None, None] == spots[None, :, :], axis=-1)
    memory_dimension = jax.random.uniform(depth_key, (TOKENS, HEADS, HEAD), jnp.float32, 0.22, 0.69)
    segment_span = jnp.where(dropped_sequence_items[:, :, None], -memory_dimension, 0.0)
    overall_aggregate = starting_index[:, None, None] + segment_span
    return overall_aggregate.reshape(TOKENS, HEADS * HEAD).astype(jnp.float32)


def draw_conv_kernel(key, part):
    base_key = jax.random.fold_in(key, 37)
    value_key = jax.random.fold_in(base_key, 0)
    rising = jnp.exp(math.log(6.0) * jnp.arange(CONV, dtype=jnp.float32) / CONV)
    entries = jnp.clip(jax.random.normal(value_key, (KW, CONV), jnp.float32), -4.0, 4.0)
    return (entries * rising / math.sqrt(KW)).astype(jnp.float32)


def block_levels(stream_key, dims, cuts, low, high):
    factor_of = 1.0
    for axis_at, parts in cuts:
        heights = jax.random.uniform(jax.random.fold_in(jax.random.fold_in(stream_key, 6), axis_at), (parts,), jnp.float32, low / len(cuts), high / len(cuts))
        factor_of = factor_of * jnp.repeat(jnp.exp(heights), dims[axis_at] // parts).reshape((-1,) + (1,) * (len(dims) - 1 - axis_at))
    return factor_of


def centred(key, dims, deviation, most, pieces=(), kind=jnp.bfloat16):
    values = deviation * jax.random.normal(key, dims, jnp.float32)
    if pieces:
        values = values * block_levels(key, dims, pieces, -0.22, 0.18)
    return jnp.clip(values, -most, most).astype(kind)


def setup_inputs(seed: int = 0) -> dict:
    key_of = jax.random.split(jax.random.key(seed), 20)
    tokens = centred(key_of[0], (TOKENS, D), 1.0, 6.0, ((0, 32),))
    norm_gain = jnp.clip(1.0 + 0.18 * jax.random.normal(key_of[1], (D,), jnp.float32), 0.1, 1.9)
    w_query = centred(key_of[2], (D, HD), D ** -0.5, 0.125, ((0, 8), (1, 4)))
    w_forget = centred(key_of[3], (D, HD), D ** -0.5, 0.125, ((0, 8), (1, 4)))
    w_input = centred(key_of[4], (D, HD), D ** -0.5, 0.125, ((0, 8), (1, 4)))
    w_outgate = centred(key_of[5], (D, HD), D ** -0.5, 0.125, ((0, 8), (1, 4)))
    w_conv_value = centred(key_of[6], (D, CONV), D ** -0.5, 0.125, ((0, 8), (1, 4)))
    w_conv_gate = centred(key_of[7], (D, CONV), D ** -0.5, 0.125, ((0, 8), (1, 4)))
    w_gate_rec = centred(key_of[8], (D, D), D ** -0.5, 0.125, ((0, 8), (1, 4)))
    w_gate_conv = centred(key_of[9], (D, D), D ** -0.5, 0.125, ((0, 8), (1, 4)))
    lower_bound = draw_lower_bound(jax.random.fold_in(key_of[19], 71), 0)
    decay_shift = draw_decay_shift(jax.random.fold_in(key_of[19], 71), 0)
    state_init = centred(key_of[12], (HEADS, HEAD, HEAD), (TOKENS ** -0.5), 0.1875, ((0, 4),), jnp.float32)
    head_gain = jnp.clip(1.0 + 0.18 * jax.random.normal(key_of[13], (HD,), jnp.float32), 0.1, 1.9)
    conv_kernel = draw_conv_kernel(jax.random.fold_in(key_of[19], 71), 0)
    channel_gain = jnp.clip(1.0 + 0.18 * jax.random.normal(key_of[15], (CONV,), jnp.float32), 0.1, 1.9)
    channel_bias = centred(key_of[16], (CONV,), 0.5, 3.0, ((0, 4),), jnp.float32)
    w_out_rec = centred(key_of[17], (HD, D), HD ** -0.5, 0.1875, ((0, 4), (1, 8)))
    w_out_conv = centred(key_of[18], (CONV, D), CONV ** -0.5, 0.1875, ((0, 4), (1, 8)))
    return dict(tokens=tokens, norm_gain=norm_gain, w_query=w_query, w_forget=w_forget, w_input=w_input, w_outgate=w_outgate, w_conv_value=w_conv_value, w_conv_gate=w_conv_gate, w_gate_rec=w_gate_rec, w_gate_conv=w_gate_conv, lower_bound=lower_bound, decay_shift=decay_shift, state_init=state_init, head_gain=head_gain, conv_kernel=conv_kernel, channel_gain=channel_gain, channel_bias=channel_bias, w_out_rec=w_out_rec, w_out_conv=w_out_conv)


EPSILON = 1e-06
highest_precision = lax.Precision.HIGHEST

def normalize_rows(values, gain_vector):
    widened = values.astype(jnp.float32)
    scale = lax.rsqrt(lax.optimization_barrier(jnp.mean(widened * widened, axis=-1, keepdims=True)) + EPSILON)
    return (widened * scale * gain_vector).astype(jnp.bfloat16)

def block_step(state, inputs):
    query, input_gate, values, log_decay = inputs
    length = query.shape[1]
    causal_masked = (jnp.arange(length)[:, None] >= jnp.arange(length)[None, :])[None, :, :, None]
    cumulative = jnp.cumsum(log_decay, axis=1)
    spread = cumulative[:, :, None, :] - cumulative[:, None, :, :]
    weight = jnp.where(causal_masked, jnp.exp(jnp.where(causal_masked, spread, 0.0)), 0.0)
    scores = jnp.einsum('htd,hsd,htsd->hts', query, input_gate, weight, precision=highest_precision)
    output = jnp.einsum('hts,hsv->htv', scores, values, precision=highest_precision)
    output = output + jnp.einsum('htd,hdv->htv', query * jnp.exp(cumulative), state, precision=highest_precision)
    final = cumulative[:, -1:, :]
    carried = jnp.exp(final[:, 0, :])[:, :, None] * state
    carried = carried + jnp.einsum('hsd,hsv->hdv', input_gate * jnp.exp(final - cumulative), values, precision=highest_precision)
    return (carried, output)

def reference(tokens, norm_gain, w_query, w_forget, w_input, w_outgate, w_conv_value, w_conv_gate, w_gate_rec, w_gate_conv, lower_bound, decay_shift, state_init, head_gain, conv_kernel, channel_gain, channel_bias, w_out_rec, w_out_conv):
    normed = normalize_rows(tokens, norm_gain)

    def project(weight):
        return jnp.dot(normed, weight, preferred_element_type=jnp.float32).astype(jnp.bfloat16)
    query_raw = project(w_query)
    forget_raw = project(w_forget)
    input_raw = project(w_input)
    outgate_raw = project(w_outgate)
    value_raw = project(w_conv_value)
    gate_raw = project(w_conv_gate)
    gate_rec_raw = project(w_gate_rec)
    gate_conv_raw = project(w_gate_conv)
    query = jax.nn.silu(query_raw.astype(jnp.float32))
    input_gate = (1.0 - lower_bound) * jax.nn.sigmoid(-forget_raw.astype(jnp.float32))
    log_decay = jnp.log1p(-input_gate) + decay_shift
    values = input_raw.astype(jnp.float32)
    block_count = TOKENS // BLOCK

    def to_blocks(array):
        return array.reshape(block_count, BLOCK, HEADS, HEAD).transpose(0, 2, 1, 3)
    unused_state, blocks_out = lax.scan(block_step, state_init, (to_blocks(query), to_blocks(input_gate), to_blocks(values), to_blocks(log_decay)))
    head_out = blocks_out.transpose(0, 2, 1, 3).reshape(TOKENS, HEADS, HEAD)
    head_out = head_out * lax.rsqrt(lax.optimization_barrier(jnp.mean(head_out * head_out, axis=-1, keepdims=True)) + EPSILON)
    head_out = head_out * head_gain.reshape(HEADS, HEAD)
    mixed_rec = (head_out.reshape(TOKENS, HEADS * HEAD) * jax.nn.silu(outgate_raw.astype(jnp.float32))).astype(jnp.bfloat16)
    gated = (value_raw.astype(jnp.float32) * jax.nn.sigmoid(gate_raw.astype(jnp.float32))).astype(jnp.bfloat16)
    extended = jnp.concatenate([jnp.zeros((KW - 1, CONV), jnp.bfloat16), gated], axis=0).astype(jnp.float32)
    conv_out = jnp.zeros((TOKENS, CONV), jnp.float32)
    for tap_index in range(KW):
        conv_out = conv_out + conv_kernel[tap_index] * extended[tap_index:tap_index + TOKENS]
    scale = lax.rsqrt(lax.optimization_barrier(jnp.mean(conv_out * conv_out, axis=1, keepdims=True)) + EPSILON)
    mixed_conv = jax.nn.silu(conv_out * scale * channel_gain + channel_bias).astype(jnp.bfloat16)
    y_rec = jnp.dot(mixed_rec, w_out_rec, preferred_element_type=jnp.float32).astype(jnp.bfloat16)
    y_conv = jnp.dot(mixed_conv, w_out_conv, preferred_element_type=jnp.float32).astype(jnp.bfloat16)
    merged = jax.nn.sigmoid(gate_rec_raw.astype(jnp.float32)) * y_rec.astype(jnp.float32)
    merged = merged + jax.nn.sigmoid(gate_conv_raw.astype(jnp.float32)) * y_conv.astype(jnp.float32)
    return merged.astype(jnp.bfloat16)
```

```python
import functools

import jax
import jax.numpy as jnp
from jax import lax
from jax.experimental import pallas as pl
from jax.experimental.pallas import tpu as pltpu
from jax.sharding import PartitionSpec as P


HEAD = 128
KW = 31
RIM = 32
CHUNK = 128
EXTRA = 16
EPSILON = 1e-06

AXES = ("sp", "tp")
f32, bf16 = jnp.float32, jnp.bfloat16
HBM = pl.BlockSpec(memory_space=pltpu.HBM)
VMEM = pl.BlockSpec(memory_space=pltpu.VMEM)
SMEM = pl.BlockSpec(memory_space=pltpu.SMEM)
NT = (((1,), (1,)), ((), ()))
TN = (((0,), (0,)), ((), ()))


def normalize_rows(values, gain_vector):
    widened = values.astype(f32)
    scale = lax.rsqrt(jnp.mean(widened * widened, axis=-1, keepdims=True) + EPSILON)
    return (widened * scale * gain_vector).astype(bf16)


class Copy:
    def __init__(self, source, row, rows, to_row, to_lane=None, flag=None):
        self.source, self.row, self.rows = source, row, rows
        self.to_row, self.to_lane, self.flag = to_row, to_lane, flag

    def run(self, act, place, sources, target, semaphore):
        source = sources[self.source]
        rows = self.to_row if isinstance(self.to_row, int) else self.to_row(*place)
        if not isinstance(rows, int):
            rows = pl.multiple_of(rows, 16)
        if self.to_lane is None:
            there = target.at[pl.ds(rows, self.rows), :]
        else:
            lane = pl.multiple_of(self.to_lane(*place), HEAD)
            there = target.at[pl.ds(rows, self.rows), pl.ds(lane, source.shape[1])]

        def go():
            here = source.at[pl.ds(self.row, self.rows), :]
            getattr(pltpu.make_async_copy(here, there, semaphore), act)()

        if self.flag is None:
            go()
        else:
            pl.when(self.flag(*place))(go)


def run_all(act, copies, place, sources, target, semaphores, first=0):
    for k, copy in enumerate(copies):
        copy.run(act, place, sources, target, semaphores.at[first + k])


def where_am_i(scalars):
    return scalars[0], scalars[1], scalars[2]


def params():
    return pltpu.CompilerParams(vmem_limit_bytes=56 * 1024 * 1024)


def cost(flops, moved):
    return pl.CostEstimate(flops=int(flops), bytes_accessed=int(moved), transcendentals=0)


def project(rows, depth, token_groups, n_tokens, weight_copies, n_weights):
    size = rows // len(token_groups)

    def body(scalars, *refs):
        tokens, refs = refs[:n_tokens], refs[n_tokens:]
        weights, refs = refs[:n_weights], refs[n_weights:]
        gated, ordered, token_v, weight_v, semaphores, out_semaphores = refs
        place = where_am_i(scalars)
        run_all("start", weight_copies, place, weights, weight_v, semaphores)
        first = len(weight_copies)
        for _, copies in token_groups:
            run_all("start", copies, place, tokens, token_v, semaphores, first)
            first += len(copies)
        run_all("wait", weight_copies, place, weights, weight_v, semaphores)
        first = len(weight_copies)
        writes = []
        for k, (start, copies) in enumerate(token_groups):
            run_all("wait", copies, place, tokens, token_v, semaphores, first)
            first += len(copies)
            block = pl.ds(pl.multiple_of(start(*place), 16), size)
            write = pltpu.make_async_copy(
                token_v.at[block, :], ordered.at[block, :], out_semaphores.at[k]
            )
            write.start()
            writes.append(write)
            raw = jnp.dot(token_v[block, :], weight_v[...], preferred_element_type=f32)
            raw = raw.astype(bf16).astype(f32)
            gated[block, :] = (raw[:, :HEAD] * jax.nn.sigmoid(raw[:, HEAD:])).astype(bf16)
        for write in writes:
            write.wait()

    n_copies = len(weight_copies) + sum(len(copies) for _, copies in token_groups)
    return pl.pallas_call(
        body,
        out_shape=(
            jax.ShapeDtypeStruct((rows, HEAD), bf16),
            jax.ShapeDtypeStruct((rows, depth), bf16),
        ),
        in_specs=[SMEM] + [HBM] * (n_tokens + n_weights),
        out_specs=(VMEM, HBM),
        scratch_shapes=[
            pltpu.VMEM((rows, depth), bf16),
            pltpu.VMEM((depth, 2 * HEAD), bf16),
            pltpu.SemaphoreType.DMA((n_copies,)),
            pltpu.SemaphoreType.DMA((len(token_groups),)),
        ],
        compiler_params=params(),
        cost_estimate=cost(2 * rows * depth * 2 * HEAD, rows * depth * 4),
        name="project",
    )


def recurrence(rows, half, n_decays):
    def body(scalars, raw, rate, *refs):
        decays, (local_out, running_query, packed) = refs[:n_decays], refs[n_decays:]
        at_or_before = lax.broadcasted_iota(
            jnp.int32, (CHUNK, CHUNK), 0
        ) >= lax.broadcasted_iota(jnp.int32, (CHUNK, CHUNK), 1)
        lower = at_or_before.astype(bf16)

        def step(side, k, carry):
            state, before = carry
            within = pl.ds(pl.multiple_of(k * CHUNK, CHUNK), CHUNK)
            block = pl.ds(pl.multiple_of(side * half + k * CHUNK, CHUNK), CHUNK)
            shift = decays[0][within, :]
            if n_decays > 1:
                shift = jnp.where(scalars[1] == side, shift, decays[1][within, :].astype(f32))
            forget = raw[block, :HEAD].astype(f32)
            values = raw[block, HEAD : 2 * HEAD]
            query = raw[block, 2 * HEAD :].astype(f32)
            query = query * jax.nn.sigmoid(query)
            gate = rate[...] * jax.nn.sigmoid(-forget)
            log_decay = jnp.log1p(-gate) + shift
            high = log_decay.astype(bf16)
            rest = log_decay - high.astype(f32)
            middle = rest.astype(bf16)
            low = (rest - middle.astype(f32)).astype(bf16)
            summed = jnp.dot(
                lower, jnp.concatenate([high, middle, low], axis=1), preferred_element_type=f32
            )
            cumulative = summed[:, :HEAD] + (summed[:, HEAD : 2 * HEAD] + summed[:, 2 * HEAD :])
            centre = cumulative[CHUNK // 2 - 1 : CHUNK // 2, :]
            final = cumulative[CHUNK - 1 :, :]
            query_scaled = query * jnp.exp(cumulative - centre)
            gate_scaled = gate * jnp.exp(centre - cumulative)
            scores = lax.dot_general(
                query_scaled.astype(bf16),
                gate_scaled.astype(bf16),
                NT,
                preferred_element_type=f32,
            )
            scores = jnp.where(at_or_before, scores, 0.0).astype(bf16)
            from_state = (query_scaled * jnp.exp(centre)).astype(bf16)
            local_out[block, :] = jnp.dot(
                scores, values, preferred_element_type=f32
            ) + lax.dot_general(from_state, state.astype(bf16), NT, preferred_element_type=f32)
            running_query[block, :] = (query_scaled * jnp.exp(centre + before)).astype(bf16)
            kept = (gate_scaled * jnp.exp(final - centre)).astype(bf16)
            added = lax.dot_general(values, kept, TN, preferred_element_type=f32)
            return state * jnp.exp(final) + added, before + final

        carry = (jnp.zeros((HEAD, HEAD), f32), jnp.zeros((1, HEAD), f32))
        for side in range(n_decays):
            carry = lax.fori_loop(
                0, half // CHUNK, functools.partial(step, side), carry, unroll=3
            )
        state, total = carry
        decay = jnp.exp(total)
        high = decay.astype(bf16).astype(f32)
        packed[:HEAD, :] = state.astype(bf16)
        row = lax.broadcasted_iota(jnp.int32, (EXTRA, HEAD), 0)
        packed[HEAD:, :] = jnp.where(
            row == 0, high, jnp.where(row == 1, decay - high, 0.0)
        ).astype(bf16)

    return pl.pallas_call(
        body,
        out_shape=(
            jax.ShapeDtypeStruct((rows, HEAD), f32),
            jax.ShapeDtypeStruct((rows, HEAD), bf16),
            jax.ShapeDtypeStruct((HEAD + EXTRA, HEAD), bf16),
        ),
        in_specs=[SMEM] + [VMEM] * (2 + n_decays),
        out_specs=(VMEM, VMEM, VMEM),
        compiler_params=params(),
        cost_estimate=cost(2 * rows * HEAD * HEAD * 50, rows * HEAD * 16),
        name="recurrence",
    )


def heads(rows, depth, weight_copies, n_weights):
    size = rows // 4

    def body(scalars, tokens, *refs):
        weights, (raw_out, outgate, weight_v, semaphores) = refs[:n_weights], refs[n_weights:]

        @pl.when(pl.program_id(0) == 0)
        def _():
            for act in ("start", "wait"):
                run_all(act, weight_copies, where_am_i(scalars), weights, weight_v, semaphores)

        raw = jnp.dot(tokens[...], weight_v[...], preferred_element_type=f32).astype(bf16)
        raw_out[...] = raw[:, : 3 * HEAD]
        outgate[...] = raw[:, 3 * HEAD :]

    return pl.pallas_call(
        body,
        grid=(rows // size,),
        out_shape=(
            jax.ShapeDtypeStruct((rows, 3 * HEAD), bf16),
            jax.ShapeDtypeStruct((rows, HEAD), bf16),
        ),
        in_specs=[SMEM, pl.BlockSpec((size, depth), lambda i: (i, 0))] + [HBM] * n_weights,
        out_specs=(
            pl.BlockSpec((size, 3 * HEAD), lambda i: (i, 0)),
            pl.BlockSpec((size, HEAD), lambda i: (i, 0)),
        ),
        scratch_shapes=[
            pltpu.VMEM((depth, 4 * HEAD), bf16),
            pltpu.SemaphoreType.DMA((len(weight_copies),)),
        ],
        compiler_params=params(),
        cost_estimate=cost(2 * rows * depth * 4 * HEAD, rows * depth * 2),
        name="heads",
    )


def convolution(rows):
    def body(gated, previous, taps, gain, bias, out, extended):
        extended[:RIM, :] = previous[...].astype(f32)
        extended[RIM:, :] = gated[...].astype(f32)

        def step(k, carry):
            base = pl.multiple_of(k * CHUNK, CHUNK)
            total = jnp.zeros((CHUNK, HEAD), f32)
            for tap in range(KW):
                window = extended[pl.ds(base + RIM - KW + 1 + tap, CHUNK), :]
                total = total + taps[tap : tap + 1, :] * window
            out[pl.ds(base, CHUNK), :] = total.astype(bf16)
            return carry

        lax.fori_loop(0, rows // CHUNK, step, 0)
        row = lax.broadcasted_iota(jnp.int32, (EXTRA, HEAD), 0)
        small = jnp.zeros((EXTRA, HEAD), f32)
        for k, part in enumerate(split_three(gain[...]) + split_three(bias[...])):
            small = jnp.where(row == k, part.astype(f32), small)
        out[rows:, :] = small.astype(bf16)

    return pl.pallas_call(
        body,
        out_shape=jax.ShapeDtypeStruct((rows + EXTRA, HEAD), bf16),
        in_specs=[VMEM] * 5,
        out_specs=VMEM,
        scratch_shapes=[pltpu.VMEM((rows + RIM, HEAD), f32)],
        compiler_params=params(),
        cost_estimate=cost(2 * rows * HEAD * KW * 200, rows * HEAD * 8),
    )


def finish(rows, n_states):
    def body(scalars, local_out, running_query, outgate, initial, head_gain, *refs):
        states, out = refs[:n_states], refs[n_states]
        state = initial[...].T
        for k in reversed(range(n_states)):
            tail = states[k][HEAD:, :].astype(f32)
            decay = tail[0:1, :] + tail[1:2, :]
            state = jnp.where(
                scalars[0] > k, state * decay + states[k][:HEAD, :].astype(f32), state
            )
        state = state.astype(bf16)
        size = min(256, rows)
        for k in range(rows // size):
            block = pl.ds(k * size, size)
            head_out = local_out[block, :] + lax.dot_general(
                running_query[block, :], state, NT, preferred_element_type=f32
            )
            scale = lax.rsqrt(jnp.mean(head_out * head_out, axis=-1, keepdims=True) + EPSILON)
            gate = outgate[block, :].astype(f32)
            out[block, :] = (
                head_out * scale * head_gain[...] * (gate * jax.nn.sigmoid(gate))
            ).astype(bf16)

    return pl.pallas_call(
        body,
        out_shape=jax.ShapeDtypeStruct((rows, HEAD), bf16),
        in_specs=[SMEM] + [VMEM] * (5 + n_states),
        out_specs=VMEM,
        compiler_params=params(),
        cost_estimate=cost(2 * rows * HEAD * HEAD * 20, rows * HEAD * 12),
        name="finish",
    )


def activate(rows, channels, groups, tail_copies, n_pieces):
    size = rows // len(groups)

    def body(scalars, *refs):
        pieces, refs = refs[:n_pieces], refs[n_pieces:]
        out, wide_v, tail_v, semaphores, tail_semaphores = refs
        place = where_am_i(scalars)
        step = pl.program_id(0)

        @pl.when(step == 0)
        def _():
            run_all("start", tail_copies, place, pieces, tail_v, tail_semaphores)
            for k, copies in enumerate(groups):
                run_all("start", copies, place, pieces, wide_v, semaphores.at[k])
            run_all("wait", tail_copies, place, pieces, tail_v, tail_semaphores)

        for k, copies in enumerate(groups):

            @pl.when(step == k)
            def _():
                run_all("wait", copies, place, pieces, wide_v, semaphores.at[k])

        block = pl.ds(pl.multiple_of(step * size, size), size)
        squares = jnp.zeros((size, HEAD), f32)
        for u in range(channels // HEAD):
            value = wide_v[block, u * HEAD : (u + 1) * HEAD].astype(f32)
            squares = squares + value * value
        scale = lax.rsqrt(jnp.sum(squares, axis=-1, keepdims=True) / channels + EPSILON)
        for u in range(channels // HEAD):
            lanes = slice(u * HEAD, (u + 1) * HEAD)
            small = tail_v[:, lanes].astype(f32)
            gain = small[0:1, :] + small[1:2, :] + small[2:3, :]
            bias = small[3:4, :] + small[4:5, :] + small[5:6, :]
            value = wide_v[block, lanes].astype(f32) * scale * gain + bias
            out[:, lanes] = (value * jax.nn.sigmoid(value)).astype(bf16)

    return pl.pallas_call(
        body,
        grid=(len(groups),),
        out_shape=jax.ShapeDtypeStruct((rows, channels), bf16),
        in_specs=[SMEM] + [HBM] * n_pieces,
        out_specs=pl.BlockSpec((size, channels), lambda i: (i, 0)),
        scratch_shapes=[
            pltpu.VMEM((rows, channels), bf16),
            pltpu.VMEM((EXTRA, channels), bf16),
            pltpu.SemaphoreType.DMA((len(groups), max(len(copies) for copies in groups))),
            pltpu.SemaphoreType.DMA((len(tail_copies),)),
        ],
        compiler_params=params(),
        cost_estimate=cost(rows * channels * 2000, rows * channels * 4),
        name="activate",
    )


def combine(rows, start, lane, depth, channels, width, wide, copies, counts):
    gate_copies, out_copies, rec_copies = copies
    n_weights, n_outs, n_rec = counts
    blocks = 3 if rows % (3 * 128) == 0 else 2
    size = rows // blocks

    def body(scalars, tokens, conv, *refs):
        weights, refs = refs[:n_weights], refs[n_weights:]
        outs, refs = refs[:n_outs], refs[n_outs:]
        rec, refs = refs[:n_rec], refs[n_rec:]
        out, gate_v, out_v, rec_v, token_v, conv_v, semaphores = refs
        place = where_am_i(scalars)
        base = start(*place)
        column = pl.multiple_of(lane(*place) * width, HEAD)
        n_gate, n_out = len(gate_copies), len(out_copies)
        last = n_gate + n_out + len(rec_copies)

        def from_row(source, target, row, count, semaphore):
            rows_there = pl.ds(pl.multiple_of(base + row, 16), count)
            return pltpu.make_async_copy(
                source.at[rows_there, :], target.at[pl.ds(row, count), :], semaphores.at[semaphore]
            )

        conv_copy = from_row(conv, conv_v, 0, rows, last)
        token_copies = [
            from_row(tokens, token_v, k * size, size, last + 1 + k) for k in range(blocks)
        ]
        run_all("start", out_copies, place, outs, out_v, semaphores, n_gate)
        conv_copy.start()
        run_all("start", rec_copies, place, rec, rec_v, semaphores, n_gate + n_out)
        run_all("start", gate_copies, place, weights, gate_v, semaphores)
        for copy in token_copies:
            copy.start()
        run_all("wait", out_copies, place, outs, out_v, semaphores, n_gate)
        conv_copy.wait()
        y_conv = jnp.dot(conv_v[...], out_v[:, width:], preferred_element_type=f32).astype(bf16)
        run_all("wait", rec_copies, place, rec, rec_v, semaphores, n_gate + n_out)
        y_rec = jnp.dot(rec_v[...], out_v[:, :width], preferred_element_type=f32).astype(bf16)
        run_all("wait", gate_copies, place, weights, gate_v, semaphores)
        for k, copy in enumerate(token_copies):
            copy.wait()
            block = slice(k * size, (k + 1) * size)
            raw = jnp.dot(token_v[block, :], gate_v[...], preferred_element_type=f32)
            raw = raw.astype(bf16).astype(f32)
            merged = jax.nn.sigmoid(raw[:, :width]) * y_rec[block, :].astype(f32)
            merged = merged + jax.nn.sigmoid(raw[:, width:]) * y_conv[block, :].astype(f32)
            if wide == width:
                out[block, :] = merged.astype(bf16)
            else:
                out[block, pl.ds(column, width)] = merged.astype(bf16)

    n_copies = sum(len(group) for group in copies) + 1 + blocks
    return pl.pallas_call(
        body,
        out_shape=jax.ShapeDtypeStruct((rows, wide), bf16),
        in_specs=[SMEM] + [HBM] * (2 + n_weights + n_outs + n_rec),
        out_specs=VMEM,
        scratch_shapes=[
            pltpu.VMEM((depth, 2 * width), bf16),
            pltpu.VMEM((channels, 2 * width), bf16),
            pltpu.VMEM((rows, channels), bf16),
            pltpu.VMEM((rows, depth), bf16),
            pltpu.VMEM((rows, channels), bf16),
            pltpu.SemaphoreType.DMA((n_copies,)),
        ],
        compiler_params=params(),
        cost_estimate=cost(2 * rows * depth * 3 * width, rows * depth * 4),
        name="combine",
    )


def beside(rows, width):
    def body(scalars, theirs, mine, out):
        out[...] = theirs[...]

    return pl.pallas_call(
        body,
        out_shape=jax.ShapeDtypeStruct((rows, 2 * width), bf16),
        grid_spec=pltpu.PrefetchScalarGridSpec(
            num_scalar_prefetch=1,
            grid=(2,),
            in_specs=[pl.BlockSpec((rows // 2, width), lambda i, scalars: (i, 0)), HBM],
            out_specs=pl.BlockSpec((rows // 2, width), lambda i, scalars: (i, 1 - scalars[1])),
        ),
        input_output_aliases={2: 0},
        compiler_params=params(),
        name="beside",
    )


def split_three(vector):
    high = vector.astype(bf16)
    rest = vector - high.astype(f32)
    middle = rest.astype(bf16)
    return [high, middle, (rest - middle.astype(f32)).astype(bf16)]


def local(
    n_sp,
    n_tp,
    tokens,
    norm_gain,
    w_query,
    w_forget,
    w_input,
    w_outgate,
    w_conv_value,
    w_conv_gate,
    w_gate_rec,
    w_gate_conv,
    lower_bound,
    decay_shift,
    state_init,
    head_gain,
    conv_kernel,
    channel_gain,
    channel_bias,
    w_out_rec,
    w_out_conv,
):
    q = w_query.shape[1] // HEAD
    nz = n_sp // q
    depth = tokens.shape[1]
    channels = w_query.shape[1] * n_tp
    shard = tokens.shape[0]
    rows = shard * n_tp * q
    half = rows // q
    width = w_gate_rec.shape[1] // q
    direct = q == 2 and n_tp == 4 and nz == 4
    assert direct or q == 1
    s, t = lax.axis_index("sp"), lax.axis_index("tp")
    z, y = s // q, s % q
    own = y * n_tp + t

    def send(value, route):
        pairs = []
        for source in range(n_sp * n_tp):
            si, ti = source // n_tp, source % n_tp
            to = route(si // q, si % q, ti)
            if to is not None:
                pairs.append((source, (to[0] * q + to[1]) * n_tp + to[2]))
        return lax.ppermute(value, AXES, pairs)

    def up(k):
        return lambda a, b, c: (a + k, b, c) if a + k < nz else None

    def middle(a, b, c):
        return (3 - a, b, c) if a in (1, 2) else None

    def outwards(a, b, c):
        return ({1: 0, 2: 3}[a], b, c) if a in (1, 2) else None

    def other_y(a, b, c):
        return (a, 1 - b, c)

    def other_x(a, b, c):
        return (a, b, c ^ 2)

    def other_core(a, b, c):
        return (a, b, c ^ 1)

    def columns(ws, which):
        return jnp.concatenate(
            [
                lax.dynamic_slice_in_dim(w, which * (w.shape[1] // q), w.shape[1] // q, 1)
                for w in ws
            ],
            axis=1,
        )

    def own_columns(ws):
        if q == 1:
            return jnp.concatenate(ws, axis=1)
        theirs = send(columns(ws, 1 - y), other_y)
        mine = columns(ws, y)
        return jnp.concatenate([mine, theirs], axis=0)

    def along_z(piece, short=False):
        if not direct:
            return [lax.all_gather(piece, "sp", axis=0, tiled=True)]
        if short:
            return [piece] + [send(piece, lambda a, b, c: (a ^ k, b, c)) for k in range(1, nz)]
        outer = send(piece, lambda a, b, c: (a ^ 1, b, c))
        inner = send(piece, middle)
        outer_2 = send(inner, outwards)
        inner_2 = send(outer, middle)
        outer_3 = send(inner_2, outwards)
        return [piece, outer, inner, outer_2, inner_2, outer_3]

    def rows_of(scale, blocks, short=False):
        if not direct:
            return [Copy(0, 0, scale * nz, 0)]

        def copy(source, block, flag, row, count, within):
            return Copy(
                source,
                row,
                count,
                lambda z, y, own: block(z) * scale + within(y),
                flag=None if flag is None else lambda z, y, own: flag(z),
            )

        def inside(z):
            return (z == 1) | (z == 2)

        def at_an_end(z):
            return (z == 0) | (z == 3)

        near, far = (lambda z: jnp.where(z < 2, 2, 1)), (lambda z: jnp.where(z < 2, 3, 0))
        sources = (
            (0, lambda z: z, None),
            (1, lambda z: z ^ 1, None),
            (2, near, inside),
            (3, near, at_an_end),
            (4, far, inside),
            (5, far, at_an_end),
        )
        if short:
            sources = [(k, lambda z, k=k: z ^ k, None) for k in range(nz)]
        return [copy(*source, *block) for source in sources for block in blocks]

    def plane_gather(value, halves=False):
        size = value.shape[0]
        if not direct:
            everything = lax.all_gather(value, "tp", axis=0, tiled=False)
            return [everything[k] for k in range(n_tp)], [(k, 0, size, 0, k) for k in range(n_tp)]
        by_y, by_x = send(value, other_y), send(value, other_x)
        if halves:
            cut = size // 2
            top = send(by_x[:cut], other_y)
            bottom = send(by_y[cut:], other_x)
            arrays, parts = [], []
            for array, row, place in (
                (value, 0, 0),
                (by_x, 0, 2),
                (by_y, 0, n_tp),
                (top, 0, n_tp + 2),
                (bottom, cut, n_tp + 2),
            ):
                for piece, core in ((array, 0), (send(array, other_core), 1)):
                    parts.append((len(arrays), 0, piece.shape[0], row, place ^ core))
                    arrays.append(piece)
            return arrays, parts
        across = send(value, lambda a, b, c: (a, 1 - b, c ^ 2))
        near = send(value, other_core)
        others = jnp.concatenate([by_x, by_y, across], axis=0)
        others = send(others, other_core)
        arrays = [value, by_x, by_y, across, near, others]
        places = (0, 2, n_tp, n_tp + 2, 1)
        parts = [(k, 0, size, 0, place) for k, place in enumerate(places)]
        parts += [(5, k * size, size, 0, place ^ 1) for k, place in enumerate(places[1:4])]
        return arrays, parts

    def absolute(place, own):
        return place ^ own if direct else place

    def token_copy(array, row, count, within, place):
        return Copy(
            array, row, count, lambda z, y, own: absolute(place, own) * shard + within
        )

    normed = normalize_rows(tokens, norm_gain)
    piece_a = own_columns((w_conv_value, w_conv_gate))
    token_arrays, token_parts = plane_gather(normed, True)
    weights_a = along_z(piece_a)
    if q == 1:
        decays = [decay_shift]
    else:
        theirs = columns((decay_shift,), 1 - y).astype(bf16)
        decays = [columns((decay_shift,), y), send(theirs, other_y)]

    def unit(vector):
        return lax.dynamic_slice_in_dim(vector, y * HEAD, HEAD, vector.ndim - 1)

    here = jnp.stack([z, y, own]).astype(jnp.int32)
    sub = depth // n_sp
    inner = [(k * sub, sub, lambda y, k=k: (y ^ k) * sub) for k in range(q)]
    token_groups = [
        (
            lambda z, y, own, k=k: (y ^ k) * half,
            [token_copy(*part) for part in token_parts if part[-1] // n_tp == k],
        )
        for k in range(q)
    ]
    gated, ordered = project(
        rows,
        depth,
        token_groups,
        len(token_arrays),
        rows_of(sub * q, inner),
        len(weights_a),
    )(here, *token_arrays, *weights_a)
    previous = send(gated[rows - RIM :], up(1))
    taps = jnp.concatenate([unit(conv_kernel), jnp.zeros((RIM - KW, HEAD), f32)])
    conv_out = convolution(rows)(
        gated, previous, taps, unit(channel_gain)[None, :], unit(channel_bias)[None, :]
    )
    conv_arrays, conv_parts = plane_gather(conv_out)

    piece_b = own_columns((w_forget, w_input, w_query, w_outgate))
    weights_b = along_z(piece_b)
    raw, outgate = heads(rows, depth, rows_of(sub * q, inner), len(weights_b))(
        here, ordered, *weights_b
    )
    local_out, running_query, packed = recurrence(rows, half, q)(
        here, raw, 1.0 - unit(lower_bound)[None, :], *decays
    )
    if direct:
        states = [send(packed, up(k)) for k in range(1, nz)]
    else:
        gathered = lax.all_gather(packed, "sp", axis=0, tiled=False)
        states = [
            lax.dynamic_index_in_dim(gathered, jnp.maximum(z - k, 0), 0, False)
            for k in range(1, nz)
        ]
    mixed_rec = finish(rows, nz - 1)(
        here,
        local_out,
        running_query,
        outgate,
        lax.dynamic_index_in_dim(state_init, y, 0, False),
        unit(head_gain)[None, :],
        *states,
    )
    rec_arrays, rec_parts = plane_gather(mixed_rec)

    gates = own_columns((w_gate_rec, w_gate_conv))
    outs = jnp.concatenate([w_out_rec, w_out_conv], axis=1)
    if direct:
        outs = send(outs, lambda a, b, c: (c, b, a))
        weights_c, weights_d = along_z(gates), along_z(outs, True)
    else:
        weights_c = along_z(gates)
        whole = [
            lax.all_gather(lax.all_gather(w, "sp", axis=1, tiled=True), "tp", axis=0, tiled=True)
            for w in (w_out_rec, w_out_conv)
        ]
        whole = [lax.dynamic_slice_in_dim(w, t * width, width, 1) for w in whole]
        weights_d = [jnp.concatenate(whole, axis=1)]

    def lane_of(place):
        def lane(z, y, own):
            block = absolute(place, own)
            return ((block % n_tp) * q + block // n_tp) * HEAD

        return lane

    n_groups = max(1, rows // 256)
    size = rows // n_groups
    groups, tail_copies = [[] for _ in range(n_groups)], []
    for array, row, count, within, place in conv_parts:
        for k in range(n_groups):
            if within <= k * size < within + count:
                groups[k].append(Copy(array, row + k * size, size, k * size, lane_of(place)))
        if within + count > rows:
            tail_copies.append(Copy(array, row + rows, EXTRA, 0, lane_of(place)))
    mixed_conv = activate(rows, channels, groups, tail_copies, len(conv_arrays))(
        here, *conv_arrays
    )

    gate_copies = rows_of(sub * q, inner)
    out_rows = channels // nz
    out_copies = rows_of(out_rows, [(0, out_rows, lambda y: 0)], True)

    def final_rows(keep):
        rec_copies = []
        for array, row, count, within, place in rec_parts:
            for side in range(q):
                if within <= side * half < within + count:
                    flag = None if q == 1 else lambda z, y, own, side=side: (y ^ keep) == side
                    rec_copies.append(
                        Copy(array, row + side * half, half, 0, lane_of(place), flag)
                    )
        return combine(
            half,
            lambda z, y, own: (y ^ keep) * half,
            lambda z, y, own: y if q > 1 and keep == 0 else 0,
            depth,
            channels,
            width,
            width * q if keep == 0 else width,
            (gate_copies, out_copies, rec_copies),
            (len(weights_c), len(weights_d), len(rec_arrays)),
        )(here, ordered, mixed_conv, *weights_c, *weights_d, *rec_arrays)

    if q == 1:
        return final_rows(0)
    theirs = send(final_rows(1), other_y)
    return beside(half, width)(here, theirs, final_rows(0))


def solution(mesh):
    in_specs = (
        P(("sp", "tp"), None),
        P(),
        P("sp", "tp"),
        P("sp", "tp"),
        P("sp", "tp"),
        P("sp", "tp"),
        P("sp", "tp"),
        P("sp", "tp"),
        P("sp", "tp"),
        P("sp", "tp"),
        P("tp"),
        P("sp", "tp"),
        P("tp", None, None),
        P("tp"),
        P(None, "tp"),
        P("tp"),
        P("tp"),
        P("tp", "sp"),
        P("tp", "sp"),
    )
    step = functools.partial(local, mesh.shape["sp"], mesh.shape["tp"])
    step = jax.shard_map(
        step, mesh=mesh, in_specs=in_specs, out_specs=P("sp", "tp"), check_vma=False
    )
    return step
```

```python
import functools

import jax
import jax.numpy as jnp
from jax import lax
from jax.experimental import pallas as pl
from jax.experimental.pallas import tpu as pltpu
from jax.sharding import PartitionSpec as P


HEAD = 128
KW = 31
RIM = 32
CHUNK = 128
EXTRA = 16
EPSILON = 1e-06

AXES = ("sp", "tp")
f32, bf16 = jnp.float32, jnp.bfloat16
HBM = pl.BlockSpec(memory_space=pltpu.HBM)
VMEM = pl.BlockSpec(memory_space=pltpu.VMEM)
SMEM = pl.BlockSpec(memory_space=pltpu.SMEM)
NT = (((1,), (1,)), ((), ()))
TN = (((0,), (0,)), ((), ()))


def normalize_rows(values, gain_vector):
    widened = values.astype(f32)
    scale = lax.rsqrt(jnp.mean(widened * widened, axis=-1, keepdims=True) + EPSILON)
    return (widened * scale * gain_vector).astype(bf16)


class Copy:
    def __init__(self, source, row, rows, to_row, to_lane=None, flag=None):
        self.source, self.row, self.rows = source, row, rows
        self.to_row, self.to_lane, self.flag = to_row, to_lane, flag

    def run(self, act, place, sources, target, semaphore):
        source = sources[self.source]
        rows = self.to_row if isinstance(self.to_row, int) else self.to_row(*place)
        if not isinstance(rows, int):
            rows = pl.multiple_of(rows, 16)
        if self.to_lane is None:
            there = target.at[pl.ds(rows, self.rows), :]
        else:
            lane = pl.multiple_of(self.to_lane(*place), HEAD)
            there = target.at[pl.ds(rows, self.rows), pl.ds(lane, source.shape[1])]

        def go():
            here = source.at[pl.ds(self.row, self.rows), :]
            getattr(pltpu.make_async_copy(here, there, semaphore), act)()

        if self.flag is None:
            go()
        else:
            pl.when(self.flag(*place))(go)


def run_all(act, copies, place, sources, target, semaphores, first=0):
    for k, copy in enumerate(copies):
        copy.run(act, place, sources, target, semaphores.at[first + k])


def where_am_i(scalars):
    return scalars[0], scalars[1], scalars[2]


def params():
    return pltpu.CompilerParams(vmem_limit_bytes=20 * 1024 * 1024)


def cost(flops, moved):
    return pl.CostEstimate(flops=int(flops), bytes_accessed=int(moved), transcendentals=0)


def project(rows, depth, token_groups, n_tokens, weight_copies, n_weights):
    size = rows // len(token_groups)

    def body(scalars, *refs):
        tokens, refs = refs[:n_tokens], refs[n_tokens:]
        weights, refs = refs[:n_weights], refs[n_weights:]
        gated, ordered, token_v, weight_v, semaphores, out_semaphores = refs
        place = where_am_i(scalars)
        run_all("start", weight_copies, place, weights, weight_v, semaphores)
        first = len(weight_copies)
        for _, copies in token_groups:
            run_all("start", copies, place, tokens, token_v, semaphores, first)
            first += len(copies)
        run_all("wait", weight_copies, place, weights, weight_v, semaphores)
        first = len(weight_copies)
        writes = []
        for k, (start, copies) in enumerate(token_groups):
            run_all("wait", copies, place, tokens, token_v, semaphores, first)
            first += len(copies)
            block = pl.ds(pl.multiple_of(start(*place), 16), size)
            write = pltpu.make_async_copy(
                token_v.at[block, :], ordered.at[block, :], out_semaphores.at[k]
            )
            write.start()
            writes.append(write)
            raw = jnp.dot(token_v[block, :], weight_v[...], preferred_element_type=f32)
            raw = raw.astype(bf16).astype(f32)
            gated[block, :] = (raw[:, :HEAD] * jax.nn.sigmoid(raw[:, HEAD:])).astype(bf16)
        for write in writes:
            write.wait()

    n_copies = len(weight_copies) + sum(len(copies) for _, copies in token_groups)
    return pl.pallas_call(
        body,
        out_shape=(
            jax.ShapeDtypeStruct((rows, HEAD), bf16),
            jax.ShapeDtypeStruct((rows, depth), bf16),
        ),
        in_specs=[SMEM] + [HBM] * (n_tokens + n_weights),
        out_specs=(VMEM, HBM),
        scratch_shapes=[
            pltpu.VMEM((rows, depth), bf16),
            pltpu.VMEM((depth, 2 * HEAD), bf16),
            pltpu.SemaphoreType.DMA((n_copies,)),
            pltpu.SemaphoreType.DMA((len(token_groups),)),
        ],
        compiler_params=params(),
        cost_estimate=cost(2 * rows * depth * 2 * HEAD, rows * depth * 4),
        name="project",
    )


def recurrence(rows, half, n_decays):
    def body(scalars, raw, rate, *refs):
        decays, (local_out, running_query, packed) = refs[:n_decays], refs[n_decays:]
        at_or_before = lax.broadcasted_iota(
            jnp.int32, (CHUNK, CHUNK), 0
        ) >= lax.broadcasted_iota(jnp.int32, (CHUNK, CHUNK), 1)
        lower = at_or_before.astype(bf16)

        def step(side, k, carry):
            state, before = carry
            within = pl.ds(pl.multiple_of(k * CHUNK, CHUNK), CHUNK)
            block = pl.ds(pl.multiple_of(side * half + k * CHUNK, CHUNK), CHUNK)
            shift = decays[0][within, :]
            if n_decays > 1:
                shift = jnp.where(scalars[1] == side, shift, decays[1][within, :].astype(f32))
            forget = raw[block, :HEAD].astype(f32)
            values = raw[block, HEAD : 2 * HEAD]
            query = raw[block, 2 * HEAD :].astype(f32)
            query = query * jax.nn.sigmoid(query)
            gate = rate[...] * jax.nn.sigmoid(-forget)
            log_decay = jnp.log1p(-gate) + shift
            high = log_decay.astype(bf16)
            rest = log_decay - high.astype(f32)
            middle = rest.astype(bf16)
            low = (rest - middle.astype(f32)).astype(bf16)
            summed = jnp.dot(
                lower, jnp.concatenate([high, middle, low], axis=1), preferred_element_type=f32
            )
            cumulative = summed[:, :HEAD] + (summed[:, HEAD : 2 * HEAD] + summed[:, 2 * HEAD :])
            centre = cumulative[CHUNK // 2 - 1 : CHUNK // 2, :]
            final = cumulative[CHUNK - 1 :, :]
            query_scaled = query * jnp.exp(cumulative - centre)
            gate_scaled = gate * jnp.exp(centre - cumulative)
            scores = lax.dot_general(
                query_scaled.astype(bf16),
                gate_scaled.astype(bf16),
                NT,
                preferred_element_type=f32,
            )
            scores = jnp.where(at_or_before, scores, 0.0).astype(bf16)
            from_state = (query_scaled * jnp.exp(centre)).astype(bf16)
            local_out[block, :] = jnp.dot(
                scores, values, preferred_element_type=f32
            ) + lax.dot_general(from_state, state.astype(bf16), NT, preferred_element_type=f32)
            running_query[block, :] = (query_scaled * jnp.exp(centre + before)).astype(bf16)
            kept = (gate_scaled * jnp.exp(final - centre)).astype(bf16)
            added = lax.dot_general(values, kept, TN, preferred_element_type=f32)
            return state * jnp.exp(final) + added, before + final

        carry = (jnp.zeros((HEAD, HEAD), f32), jnp.zeros((1, HEAD), f32))
        for side in range(n_decays):
            carry = lax.fori_loop(
                0, half // CHUNK, functools.partial(step, side), carry, unroll=6
            )
        state, total = carry
        decay = jnp.exp(total)
        high = decay.astype(bf16).astype(f32)
        packed[:HEAD, :] = state.astype(bf16)
        row = lax.broadcasted_iota(jnp.int32, (EXTRA, HEAD), 0)
        packed[HEAD:, :] = jnp.where(
            row == 0, high, jnp.where(row == 1, decay - high, 0.0)
        ).astype(bf16)

    return pl.pallas_call(
        body,
        out_shape=(
            jax.ShapeDtypeStruct((rows, HEAD), f32),
            jax.ShapeDtypeStruct((rows, HEAD), bf16),
            jax.ShapeDtypeStruct((HEAD + EXTRA, HEAD), bf16),
        ),
        in_specs=[SMEM] + [VMEM] * (2 + n_decays),
        out_specs=(VMEM, VMEM, VMEM),
        compiler_params=params(),
        cost_estimate=cost(2 * rows * HEAD * HEAD * 50, rows * HEAD * 16),
        name="recurrence",
    )


def heads(rows, depth, weight_copies, n_weights):
    size = rows // 2

    def body(scalars, tokens, *refs):
        weights, (raw_out, outgate, weight_v, semaphores) = refs[:n_weights], refs[n_weights:]

        @pl.when(pl.program_id(0) == 0)
        def _():
            for act in ("start", "wait"):
                run_all(act, weight_copies, where_am_i(scalars), weights, weight_v, semaphores)

        raw = jnp.dot(tokens[...], weight_v[...], preferred_element_type=f32).astype(bf16)
        raw_out[...] = raw[:, : 3 * HEAD]
        outgate[...] = raw[:, 3 * HEAD :]

    return pl.pallas_call(
        body,
        grid=(rows // size,),
        out_shape=(
            jax.ShapeDtypeStruct((rows, 3 * HEAD), bf16),
            jax.ShapeDtypeStruct((rows, HEAD), bf16),
        ),
        in_specs=[SMEM, pl.BlockSpec((size, depth), lambda i: (i, 0))] + [HBM] * n_weights,
        out_specs=(
            pl.BlockSpec((size, 3 * HEAD), lambda i: (i, 0)),
            pl.BlockSpec((size, HEAD), lambda i: (i, 0)),
        ),
        scratch_shapes=[
            pltpu.VMEM((depth, 4 * HEAD), bf16),
            pltpu.SemaphoreType.DMA((len(weight_copies),)),
        ],
        compiler_params=params(),
        cost_estimate=cost(2 * rows * depth * 4 * HEAD, rows * depth * 2),
        name="heads",
    )


def convolution(rows):
    def body(gated, previous, taps, gain, bias, out, extended):
        extended[:RIM, :] = previous[...].astype(f32)
        extended[RIM:, :] = gated[...].astype(f32)

        def step(k, carry):
            base = pl.multiple_of(k * CHUNK, CHUNK)
            total = jnp.zeros((CHUNK, HEAD), f32)
            for tap in range(KW):
                window = extended[pl.ds(base + RIM - KW + 1 + tap, CHUNK), :]
                total = total + taps[tap : tap + 1, :] * window
            out[pl.ds(base, CHUNK), :] = total.astype(bf16)
            return carry

        lax.fori_loop(0, rows // CHUNK, step, 0)
        row = lax.broadcasted_iota(jnp.int32, (EXTRA, HEAD), 0)
        small = jnp.zeros((EXTRA, HEAD), f32)
        for k, part in enumerate(split_three(gain[...]) + split_three(bias[...])):
            small = jnp.where(row == k, part.astype(f32), small)
        out[rows:, :] = small.astype(bf16)

    return pl.pallas_call(
        body,
        out_shape=jax.ShapeDtypeStruct((rows + EXTRA, HEAD), bf16),
        in_specs=[VMEM] * 5,
        out_specs=VMEM,
        scratch_shapes=[pltpu.VMEM((rows + RIM, HEAD), f32)],
        compiler_params=params(),
        cost_estimate=cost(2 * rows * HEAD * KW * 200, rows * HEAD * 8),
    )


def finish(rows, n_states):
    def body(scalars, local_out, running_query, outgate, initial, head_gain, *refs):
        states, out = refs[:n_states], refs[n_states]
        state = initial[...].T
        for k in reversed(range(n_states)):
            tail = states[k][HEAD:, :].astype(f32)
            decay = tail[0:1, :] + tail[1:2, :]
            state = jnp.where(
                scalars[0] > k, state * decay + states[k][:HEAD, :].astype(f32), state
            )
        state = state.astype(bf16)
        size = min(256, rows)
        for k in range(rows // size):
            block = pl.ds(k * size, size)
            head_out = local_out[block, :] + lax.dot_general(
                running_query[block, :], state, NT, preferred_element_type=f32
            )
            scale = lax.rsqrt(jnp.mean(head_out * head_out, axis=-1, keepdims=True) + EPSILON)
            gate = outgate[block, :].astype(f32)
            out[block, :] = (
                head_out * scale * head_gain[...] * (gate * jax.nn.sigmoid(gate))
            ).astype(bf16)

    return pl.pallas_call(
        body,
        out_shape=jax.ShapeDtypeStruct((rows, HEAD), bf16),
        in_specs=[SMEM] + [VMEM] * (5 + n_states),
        out_specs=VMEM,
        compiler_params=params(),
        cost_estimate=cost(2 * rows * HEAD * HEAD * 20, rows * HEAD * 12),
        name="finish",
    )


def activate(rows, channels, groups, tail_copies, n_pieces):
    size = rows // len(groups)

    def body(scalars, *refs):
        pieces, refs = refs[:n_pieces], refs[n_pieces:]
        out, wide_v, tail_v, semaphores, tail_semaphores = refs
        place = where_am_i(scalars)
        step = pl.program_id(0)

        @pl.when(step == 0)
        def _():
            run_all("start", tail_copies, place, pieces, tail_v, tail_semaphores)
            for k, copies in enumerate(groups):
                run_all("start", copies, place, pieces, wide_v, semaphores.at[k])
            run_all("wait", tail_copies, place, pieces, tail_v, tail_semaphores)

        for k, copies in enumerate(groups):

            @pl.when(step == k)
            def _():
                run_all("wait", copies, place, pieces, wide_v, semaphores.at[k])

        block = pl.ds(pl.multiple_of(step * size, size), size)
        squares = jnp.zeros((size, HEAD), f32)
        for u in range(channels // HEAD):
            value = wide_v[block, u * HEAD : (u + 1) * HEAD].astype(f32)
            squares = squares + value * value
        scale = lax.rsqrt(jnp.sum(squares, axis=-1, keepdims=True) / channels + EPSILON)
        for u in range(channels // HEAD):
            lanes = slice(u * HEAD, (u + 1) * HEAD)
            small = tail_v[:, lanes].astype(f32)
            gain = small[0:1, :] + small[1:2, :] + small[2:3, :]
            bias = small[3:4, :] + small[4:5, :] + small[5:6, :]
            value = wide_v[block, lanes].astype(f32) * scale * gain + bias
            out[:, lanes] = (value * jax.nn.sigmoid(value)).astype(bf16)

    return pl.pallas_call(
        body,
        grid=(len(groups),),
        out_shape=jax.ShapeDtypeStruct((rows, channels), bf16),
        in_specs=[SMEM] + [HBM] * n_pieces,
        out_specs=pl.BlockSpec((size, channels), lambda i: (i, 0)),
        scratch_shapes=[
            pltpu.VMEM((rows, channels), bf16),
            pltpu.VMEM((EXTRA, channels), bf16),
            pltpu.SemaphoreType.DMA((len(groups), max(len(copies) for copies in groups))),
            pltpu.SemaphoreType.DMA((len(tail_copies),)),
        ],
        compiler_params=params(),
        cost_estimate=cost(rows * channels * 2000, rows * channels * 4),
        name="activate",
    )


def combine(rows, start, lane, depth, channels, width, wide, copies, counts):
    gate_copies, out_copies, rec_copies = copies
    n_weights, n_outs, n_rec = counts
    blocks = 2
    size = rows // blocks

    def body(scalars, tokens, conv, *refs):
        weights, refs = refs[:n_weights], refs[n_weights:]
        outs, refs = refs[:n_outs], refs[n_outs:]
        rec, refs = refs[:n_rec], refs[n_rec:]
        out, gate_v, out_v, rec_v, token_v, conv_v, semaphores = refs
        place = where_am_i(scalars)
        base = start(*place)
        column = pl.multiple_of(lane(*place) * width, HEAD)
        n_gate, n_out = len(gate_copies), len(out_copies)
        last = n_gate + n_out + len(rec_copies)

        def from_row(source, target, row, count, semaphore):
            rows_there = pl.ds(pl.multiple_of(base + row, 16), count)
            return pltpu.make_async_copy(
                source.at[rows_there, :], target.at[pl.ds(row, count), :], semaphores.at[semaphore]
            )

        conv_copy = from_row(conv, conv_v, 0, rows, last)
        token_copies = [
            from_row(tokens, token_v, k * size, size, last + 1 + k) for k in range(blocks)
        ]
        run_all("start", out_copies, place, outs, out_v, semaphores, n_gate)
        conv_copy.start()
        run_all("start", rec_copies, place, rec, rec_v, semaphores, n_gate + n_out)
        run_all("start", gate_copies, place, weights, gate_v, semaphores)
        for copy in token_copies:
            copy.start()
        run_all("wait", out_copies, place, outs, out_v, semaphores, n_gate)
        conv_copy.wait()
        y_conv = jnp.dot(conv_v[...], out_v[:, width:], preferred_element_type=f32).astype(bf16)
        run_all("wait", rec_copies, place, rec, rec_v, semaphores, n_gate + n_out)
        y_rec = jnp.dot(rec_v[...], out_v[:, :width], preferred_element_type=f32).astype(bf16)
        run_all("wait", gate_copies, place, weights, gate_v, semaphores)
        for k, copy in enumerate(token_copies):
            copy.wait()
            block = slice(k * size, (k + 1) * size)
            raw = jnp.dot(token_v[block, :], gate_v[...], preferred_element_type=f32)
            raw = raw.astype(bf16).astype(f32)
            merged = jax.nn.sigmoid(raw[:, :width]) * y_rec[block, :].astype(f32)
            merged = merged + jax.nn.sigmoid(raw[:, width:]) * y_conv[block, :].astype(f32)
            if wide == width:
                out[block, :] = merged.astype(bf16)
            else:
                out[block, pl.ds(column, width)] = merged.astype(bf16)

    n_copies = sum(len(group) for group in copies) + 1 + blocks
    return pl.pallas_call(
        body,
        out_shape=jax.ShapeDtypeStruct((rows, wide), bf16),
        in_specs=[SMEM] + [HBM] * (2 + n_weights + n_outs + n_rec),
        out_specs=VMEM,
        scratch_shapes=[
            pltpu.VMEM((depth, 2 * width), bf16),
            pltpu.VMEM((channels, 2 * width), bf16),
            pltpu.VMEM((rows, channels), bf16),
            pltpu.VMEM((rows, depth), bf16),
            pltpu.VMEM((rows, channels), bf16),
            pltpu.SemaphoreType.DMA((n_copies,)),
        ],
        compiler_params=params(),
        cost_estimate=cost(2 * rows * depth * 3 * width, rows * depth * 4),
        name="combine",
    )


def beside(rows, width):
    def body(scalars, theirs, mine, out):
        out[...] = theirs[...]

    return pl.pallas_call(
        body,
        out_shape=jax.ShapeDtypeStruct((rows, 2 * width), bf16),
        grid_spec=pltpu.PrefetchScalarGridSpec(
            num_scalar_prefetch=1,
            grid=(1,),
            in_specs=[pl.BlockSpec((rows, width), lambda i, scalars: (i, 0)), HBM],
            out_specs=pl.BlockSpec((rows, width), lambda i, scalars: (i, 1 - scalars[1])),
        ),
        input_output_aliases={2: 0},
        compiler_params=params(),
        name="beside",
    )


def split_three(vector):
    high = vector.astype(bf16)
    rest = vector - high.astype(f32)
    middle = rest.astype(bf16)
    return [high, middle, (rest - middle.astype(f32)).astype(bf16)]


def local(
    n_sp,
    n_tp,
    tokens,
    norm_gain,
    w_query,
    w_forget,
    w_input,
    w_outgate,
    w_conv_value,
    w_conv_gate,
    w_gate_rec,
    w_gate_conv,
    lower_bound,
    decay_shift,
    state_init,
    head_gain,
    conv_kernel,
    channel_gain,
    channel_bias,
    w_out_rec,
    w_out_conv,
):
    q = w_query.shape[1] // HEAD
    nz = n_sp // q
    depth = tokens.shape[1]
    channels = w_query.shape[1] * n_tp
    shard = tokens.shape[0]
    rows = shard * n_tp * q
    half = rows // q
    width = w_gate_rec.shape[1] // q
    direct = q == 2 and n_tp == 4 and nz == 4
    assert direct or q == 1
    s, t = lax.axis_index("sp"), lax.axis_index("tp")
    z, y = s // q, s % q
    own = y * n_tp + t

    def send(value, route):
        pairs = []
        for source in range(n_sp * n_tp):
            si, ti = source // n_tp, source % n_tp
            to = route(si // q, si % q, ti)
            if to is not None:
                pairs.append((source, (to[0] * q + to[1]) * n_tp + to[2]))
        return lax.ppermute(value, AXES, pairs)

    def up(k):
        return lambda a, b, c: (a + k, b, c) if a + k < nz else None

    def middle(a, b, c):
        return (3 - a, b, c) if a in (1, 2) else None

    def outwards(a, b, c):
        return ({1: 0, 2: 3}[a], b, c) if a in (1, 2) else None

    def other_y(a, b, c):
        return (a, 1 - b, c)

    def other_x(a, b, c):
        return (a, b, c ^ 2)

    def other_core(a, b, c):
        return (a, b, c ^ 1)

    def columns(ws, which):
        return jnp.concatenate(
            [
                lax.dynamic_slice_in_dim(w, which * (w.shape[1] // q), w.shape[1] // q, 1)
                for w in ws
            ],
            axis=1,
        )

    def own_columns(ws):
        if q == 1:
            return jnp.concatenate(ws, axis=1)
        theirs = send(columns(ws, 1 - y), other_y)
        mine = columns(ws, y)
        return jnp.concatenate([mine, theirs], axis=0)

    def along_z(piece, short=False):
        if not direct:
            return [lax.all_gather(piece, "sp", axis=0, tiled=True)]
        if short:
            return [piece] + [send(piece, lambda a, b, c: (a ^ k, b, c)) for k in range(1, nz)]
        outer = send(piece, lambda a, b, c: (a ^ 1, b, c))
        inner = send(piece, middle)
        outer_2 = send(inner, outwards)
        inner_2 = send(outer, middle)
        outer_3 = send(inner_2, outwards)
        return [piece, outer, inner, outer_2, inner_2, outer_3]

    def rows_of(scale, blocks, short=False):
        if not direct:
            return [Copy(0, 0, scale * nz, 0)]

        def copy(source, block, flag, row, count, within):
            return Copy(
                source,
                row,
                count,
                lambda z, y, own: block(z) * scale + within(y),
                flag=None if flag is None else lambda z, y, own: flag(z),
            )

        def inside(z):
            return (z == 1) | (z == 2)

        def at_an_end(z):
            return (z == 0) | (z == 3)

        near, far = (lambda z: jnp.where(z < 2, 2, 1)), (lambda z: jnp.where(z < 2, 3, 0))
        sources = (
            (0, lambda z: z, None),
            (1, lambda z: z ^ 1, None),
            (2, near, inside),
            (3, near, at_an_end),
            (4, far, inside),
            (5, far, at_an_end),
        )
        if short:
            sources = [(k, lambda z, k=k: z ^ k, None) for k in range(nz)]
        return [copy(*source, *block) for source in sources for block in blocks]

    def plane_gather(value, halves=False):
        size = value.shape[0]
        if not direct:
            everything = lax.all_gather(value, "tp", axis=0, tiled=False)
            return [everything[k] for k in range(n_tp)], [(k, 0, size, 0, k) for k in range(n_tp)]
        by_y, by_x = send(value, other_y), send(value, other_x)
        if halves:
            cut = size // 2
            top = send(by_x[:cut], other_y)
            bottom = send(by_y[cut:], other_x)
            arrays, parts = [], []
            for array, row, place in (
                (value, 0, 0),
                (by_x, 0, 2),
                (by_y, 0, n_tp),
                (top, 0, n_tp + 2),
                (bottom, cut, n_tp + 2),
            ):
                for piece, core in ((array, 0), (send(array, other_core), 1)):
                    parts.append((len(arrays), 0, piece.shape[0], row, place ^ core))
                    arrays.append(piece)
            return arrays, parts
        across = send(value, lambda a, b, c: (a, 1 - b, c ^ 2))
        near = send(value, other_core)
        others = jnp.concatenate([by_x, by_y, across], axis=0)
        others = send(others, other_core)
        arrays = [value, by_x, by_y, across, near, others]
        places = (0, 2, n_tp, n_tp + 2, 1)
        parts = [(k, 0, size, 0, place) for k, place in enumerate(places)]
        parts += [(5, k * size, size, 0, place ^ 1) for k, place in enumerate(places[1:4])]
        return arrays, parts

    def absolute(place, own):
        return place ^ own if direct else place

    def token_copy(array, row, count, within, place):
        return Copy(
            array, row, count, lambda z, y, own: absolute(place, own) * shard + within
        )

    normed = normalize_rows(tokens, norm_gain)
    piece_a = own_columns((w_conv_value, w_conv_gate))
    token_arrays, token_parts = plane_gather(normed, True)
    weights_a = along_z(piece_a)
    if q == 1:
        decays = [decay_shift]
    else:
        theirs = columns((decay_shift,), 1 - y).astype(bf16)
        decays = [columns((decay_shift,), y), send(theirs, other_y)]

    def unit(vector):
        return lax.dynamic_slice_in_dim(vector, y * HEAD, HEAD, vector.ndim - 1)

    here = jnp.stack([z, y, own]).astype(jnp.int32)
    sub = depth // n_sp
    inner = [(k * sub, sub, lambda y, k=k: (y ^ k) * sub) for k in range(q)]
    token_groups = [
        (
            lambda z, y, own, k=k: (y ^ k) * half,
            [token_copy(*part) for part in token_parts if part[-1] // n_tp == k],
        )
        for k in range(q)
    ]
    gated, ordered = project(
        rows,
        depth,
        token_groups,
        len(token_arrays),
        rows_of(sub * q, inner),
        len(weights_a),
    )(here, *token_arrays, *weights_a)
    previous = send(gated[rows - RIM :], up(1))
    taps = jnp.concatenate([unit(conv_kernel), jnp.zeros((RIM - KW, HEAD), f32)])
    conv_out = convolution(rows)(
        gated, previous, taps, unit(channel_gain)[None, :], unit(channel_bias)[None, :]
    )
    conv_arrays, conv_parts = plane_gather(conv_out)

    piece_b = own_columns((w_forget, w_input, w_query, w_outgate))
    weights_b = along_z(piece_b)
    raw, outgate = heads(rows, depth, rows_of(sub * q, inner), len(weights_b))(
        here, ordered, *weights_b
    )
    local_out, running_query, packed = recurrence(rows, half, q)(
        here, raw, 1.0 - unit(lower_bound)[None, :], *decays
    )
    if direct:
        states = [send(packed, up(k)) for k in range(1, nz)]
    else:
        gathered = lax.all_gather(packed, "sp", axis=0, tiled=False)
        states = [
            lax.dynamic_index_in_dim(gathered, jnp.maximum(z - k, 0), 0, False)
            for k in range(1, nz)
        ]
    mixed_rec = finish(rows, nz - 1)(
        here,
        local_out,
        running_query,
        outgate,
        lax.dynamic_index_in_dim(state_init, y, 0, False),
        unit(head_gain)[None, :],
        *states,
    )
    rec_arrays, rec_parts = plane_gather(mixed_rec)

    gates = own_columns((w_gate_rec, w_gate_conv))
    outs = jnp.concatenate([w_out_rec, w_out_conv], axis=1)
    if direct:
        outs = send(outs, lambda a, b, c: (c, b, a))
        weights_c, weights_d = along_z(gates), along_z(outs, True)
    else:
        weights_c = along_z(gates)
        whole = [
            lax.all_gather(lax.all_gather(w, "sp", axis=1, tiled=True), "tp", axis=0, tiled=True)
            for w in (w_out_rec, w_out_conv)
        ]
        whole = [lax.dynamic_slice_in_dim(w, t * width, width, 1) for w in whole]
        weights_d = [jnp.concatenate(whole, axis=1)]

    def lane_of(place):
        def lane(z, y, own):
            block = absolute(place, own)
            return ((block % n_tp) * q + block // n_tp) * HEAD

        return lane

    n_groups = max(1, rows // 256)
    size = rows // n_groups
    groups, tail_copies = [[] for _ in range(n_groups)], []
    for array, row, count, within, place in conv_parts:
        for k in range(n_groups):
            if within <= k * size < within + count:
                groups[k].append(Copy(array, row + k * size, size, k * size, lane_of(place)))
        if within + count > rows:
            tail_copies.append(Copy(array, row + rows, EXTRA, 0, lane_of(place)))
    mixed_conv = activate(rows, channels, groups, tail_copies, len(conv_arrays))(
        here, *conv_arrays
    )

    gate_copies = rows_of(sub * q, inner)
    out_rows = channels // nz
    out_copies = rows_of(out_rows, [(0, out_rows, lambda y: 0)], True)

    def final_rows(keep):
        rec_copies = []
        for array, row, count, within, place in rec_parts:
            for side in range(q):
                if within <= side * half < within + count:
                    flag = None if q == 1 else lambda z, y, own, side=side: (y ^ keep) == side
                    rec_copies.append(
                        Copy(array, row + side * half, half, 0, lane_of(place), flag)
                    )
        return combine(
            half,
            lambda z, y, own: (y ^ keep) * half,
            lambda z, y, own: y if q > 1 and keep == 0 else 0,
            depth,
            channels,
            width,
            width * q if keep == 0 else width,
            (gate_copies, out_copies, rec_copies),
            (len(weights_c), len(weights_d), len(rec_arrays)),
        )(here, ordered, mixed_conv, *weights_c, *weights_d, *rec_arrays)

    if q == 1:
        return final_rows(0)
    theirs = send(final_rows(1), other_y)
    return beside(half, width)(here, theirs, final_rows(0))


def solution(mesh):
    in_specs = (
        P(("sp", "tp"), None),
        P(),
        P("sp", "tp"),
        P("sp", "tp"),
        P("sp", "tp"),
        P("sp", "tp"),
        P("sp", "tp"),
        P("sp", "tp"),
        P("sp", "tp"),
        P("sp", "tp"),
        P("tp"),
        P("sp", "tp"),
        P("tp", None, None),
        P("tp"),
        P(None, "tp"),
        P("tp"),
        P("tp"),
        P("tp", "sp"),
        P("tp", "sp"),
    )
    step = functools.partial(local, mesh.shape["sp"], mesh.shape["tp"])
    step = jax.shard_map(
        step, mesh=mesh, in_specs=in_specs, out_specs=P("sp", "tp"), check_vma=False
    )
    return step
```
